256 devices in a mesh: grp: 2 (over z), ep: 64 (over y, x), tp: 2 (over core).
Axes of the slice: x: 8, y: 8, z: 2, core: 2. Of those that a mesh axis runs over, the one named last changes fastest.
The devices are a block of a 8x8x16 slice.
Arguments:
- tokens_in: bfloat16 [8192, 2048], P(('grp', 'ep')), parts along dimension 0, may hold values from -6 to 6
- norm_gain: float32 [2048], replicated, may hold values from 0.1 to 1.9
- gate_proj: bfloat16 [64, 2048, 1024], P('ep', None, 'tp'), may hold values from -0.125 to 0.125
- up_proj: bfloat16 [64, 2048, 1024], P('ep', None, 'tp'), may hold values from -0.125 to 0.125
- down_proj: bfloat16 [64, 1024, 2048], P('ep', 'tp'), may hold values from -0.1875 to 0.1875
- route_ids: int32 [8192, 8], P(('grp', 'ep')), parts along dimension 0, may hold values from 0 to 63, all different within a row; in each aligned block of 64 rows (0 to 63, 64 to 127, ...) at most 16 rows name the same one
- group_weight: float32 [8192, 8], P(('grp', 'ep')), parts along dimension 0, may hold values from 0.05 to 1
- expert_weight: float32 [8192, 8], P(('grp', 'ep')), parts along dimension 0, may hold values from 0.05 to 1
Outputs:
- expert_mix: bfloat16 [8192, 2048], P(('grp', 'ep'), 'tp'), parts along dimension 0
The draws below stay inside these ranges and needn't reach their ends.
There are 2 independent parts, one for each index of `grp`. The reference program is written for one: setup_inputs(seed, part) draws one part's arguments, and reference() takes and returns one part's arrays. A program takes and returns all parts, laid end to end along the dimension named above; an argument that names none is the same for every part. Nothing has to cross between parts.
Inputs may be any that keep to these rules, and one draw needn't show every extreme that they name: `route_ids`: each row names 8 different experts; within the rows of one index of ep no expert is named by more than 16 rows, a bound that some of them reach.
All inputs are finite; a program needn't handle non-finite values.
Results may differ from the reference program's by a relative error of at most 0.0077.
Values may be sent and summed in bfloat16 or wider, within the bound.
No kernel may reach another device: no remote copies, remote signals or barrier semaphores. Data moves between devices by JAX's collectives and lax.ppermute only.
A program may use at most 64 MiB of HBM per device.

```python
import math
import jax
import jax.numpy as jnp
import numpy as np
from jax import lax

D = 2048
DE = 1024
TOP = 8
EXP_GRP = 8
TOK_DEV = 64
EXPERTS = 64
GROUPS = 8
CAP = 16
TOKENS = 4096
N_EP = 64
N_TP = 2


def steps_of(own_key, dims, shards, smallest, largest):
    loudness = 1.0
    for axis_at, shards_of in shards:
        draws = jax.random.uniform(jax.random.fold_in(jax.random.fold_in(own_key, 6), axis_at), (shards_of,), jnp.float32, smallest / len(shards), largest / len(shards))
        loudness = loudness * jnp.repeat(jnp.exp(draws), dims[axis_at] // shards_of).reshape((-1,) + (1,) * (len(dims) - 1 - axis_at))
    return loudness


def shared_out(key, own, number, rows, count, top, most, skew):
    ranking = jax.random.permutation(key, count)
    crowded, usual = load_shares(count, rows * top, most, skew, True), load_shares(count, rows * top, most, skew, False)
    places = jnp.arange(count)

    def named(sizes, offset_by):
        used = int((sizes > 0).sum())
        fixed = max(1, used // 4)
        passed = fixed + (places - fixed + offset_by * (used - fixed)) % max(1, count - fixed)
        return jnp.zeros((count,), jnp.int32).at[ranking[jnp.where(places < fixed, places, passed)]].set(jnp.asarray(sizes, jnp.int32))

    sizes = jnp.where(number % 4 == 0, named(crowded, number // 4), named(usual, number - number // 4 - 1))
    mixed = jax.random.permutation(jax.random.fold_in(own, 3), count)
    giver, receiver = mixed[0:count // 2 * 2:2], mixed[1:count // 2 * 2:2]
    margin = jnp.minimum(sizes[giver] - 1, most - sizes[receiver]) // 2
    margin = jnp.where((giver == ranking[0]) | (receiver == ranking[0]) | (sizes[receiver] == 0), 0, jnp.maximum(margin, 0))
    passed = jax.random.randint(jax.random.fold_in(own, 4), (count // 2,), 0, 1 << 20) % (margin + 1)
    sizes = sizes.at[giver].add(-passed).at[receiver].add(passed)
    labels = jnp.searchsorted(jnp.cumsum(sizes), jnp.arange(rows * top), side="right").astype(jnp.int32)
    grid = labels.reshape(top, rows).T
    grid = grid[jax.random.permutation(jax.random.fold_in(own, 1), rows)]
    offset_by = jax.random.randint(jax.random.fold_in(own, 2), (rows, 1), 0, top)
    return jnp.take_along_axis(grid, (jnp.arange(top)[None, :] + offset_by) % top, axis=1)


def load_shares(number_of, total, limit, skew, full):
    portions = [(1 << 20) // math.isqrt(standing ** skew) + 1 for standing in range(1, number_of + 1)]
    largest = limit if full else min(limit, max(-(-total // number_of), total * portions[0] // sum(portions)))
    least = 1 if total - largest >= number_of - 1 else 0
    given, spare = [largest] + [least] * (number_of - 1), total - largest - least * (number_of - 1)
    while spare > 0:
        free = [i for i in range(1, number_of) if given[i] < largest] or [i for i in range(1, number_of) if given[i] < limit]
        mass, left = sum([portions[i] for i in free]), spare
        for i in free:
            addition = min(limit - given[i], max(1, left * portions[i] // mass), spare)
            given[i] = given[i] + addition
            spare = spare - addition
    return np.array(given)


def noise(stream_key, dims, deviation, limit, split=(), kind=jnp.bfloat16):
    drawn = jax.random.normal(stream_key, dims, jnp.float32) * deviation
    if len(split) > 0:
        drawn = steps_of(stream_key, dims, split, -0.22, 0.18) * drawn
    return jnp.clip(drawn, min=-limit, max=limit).astype(kind)


def setup_inputs(seed: int = 0, part: int = 0) -> dict:
    arg_keys = jax.random.split(jax.random.key(seed), 9)
    own_keys = jax.random.split(jax.random.fold_in(arg_keys[8], part), 9)
    tokens_in = noise(own_keys[0], (TOKENS, D), 1.0, 6.0, ((0, 64),))
    norm_gain = jnp.clip(1.0 + 0.18 * jax.random.normal(arg_keys[1], (D,), jnp.float32), 0.1, 1.9)
    gate_proj = noise(arg_keys[2], (EXPERTS, D, DE), D ** -0.5, 0.125, ((0, 64), (2, 2)))
    up_proj = noise(arg_keys[3], (EXPERTS, D, DE), D ** -0.5, 0.125, ((0, 64), (2, 2)))
    down_proj = noise(arg_keys[4], (EXPERTS, DE, D), DE ** -0.5, 0.1875, ((0, 64), (1, 2)))
    route_ids_keys = jax.random.split(jax.random.fold_in(own_keys[5], 1), TOKENS // TOK_DEV)
    route_ids_turns = jax.random.permutation(jax.random.fold_in(own_keys[5], 3), TOKENS // TOK_DEV)
    route_ids = jax.vmap(lambda own, number: shared_out(jax.random.fold_in(own_keys[5], 2), own, number, TOK_DEV, EXPERTS, TOP, CAP, 2))(route_ids_keys, route_ids_turns).reshape((TOKENS, TOP))
    group_weight = jnp.clip(jnp.exp(math.log(1.0) - 2.9957323 * jax.random.uniform(own_keys[6], (TOKENS, GROUPS), jnp.float32) ** steps_of(own_keys[6], (TOKENS, GROUPS), ((0, 64),), -0.2, 0.2)), 0.05, 1.0)
    expert_weight = jnp.clip(jnp.exp(math.log(1.0) - 2.9957323 * jax.random.uniform(own_keys[7], (TOKENS, TOP), jnp.float32) ** steps_of(own_keys[7], (TOKENS, TOP), ((0, 64),), -0.2, 0.2)), 0.05, 1.0)
    return dict(tokens_in=tokens_in, norm_gain=norm_gain, gate_proj=gate_proj, up_proj=up_proj, down_proj=down_proj, route_ids=route_ids, group_weight=group_weight, expert_weight=expert_weight)


EPSILON = 1e-06

def reference(tokens_in, norm_gain, gate_proj, up_proj, down_proj, route_ids, group_weight, expert_weight):
    row_values = tokens_in.astype(jnp.float32)
    inv_scale = lax.rsqrt(lax.optimization_barrier(jnp.mean(row_values * row_values, axis=-1, keepdims=True)) + EPSILON)
    normed = (row_values * inv_scale * norm_gain.astype(jnp.float32)).astype(jnp.bfloat16)
    token_count = tokens_in.shape[0]
    expert_count = gate_proj.shape[0]
    route_count = token_count * TOP
    flat_ids = route_ids.reshape(route_count).astype(jnp.int32)
    sort_order = jnp.argsort(flat_ids, stable=True).astype(jnp.int32)
    expert_counts = lax.optimization_barrier(jnp.sum((flat_ids[None, :] == jnp.arange(expert_count, dtype=jnp.int32)[:, None]).astype(jnp.int32), axis=1)).astype(jnp.int32)
    expert_starts = (jnp.cumsum(expert_counts) - expert_counts).astype(jnp.int32)
    buffer_rows = N_EP * CAP
    padded_order = jnp.concatenate([sort_order, jnp.zeros((buffer_rows,), jnp.int32)])
    half_width = DE // N_TP

    def one_expert(expert_index):
        begin_at = expert_starts[expert_index].astype(jnp.int32)
        picked = lax.dynamic_slice_in_dim(padded_order, begin_at, buffer_rows)
        is_valid = jnp.arange(buffer_rows, dtype=jnp.int32) < expert_counts[expert_index]
        source_rows = normed[picked // TOP]
        gate_acts = jnp.dot(source_rows, gate_proj[expert_index], preferred_element_type=jnp.float32)
        up_acts = jnp.dot(source_rows, up_proj[expert_index], preferred_element_type=jnp.float32)
        hidden = (jax.nn.silu(gate_acts) * up_acts).astype(jnp.bfloat16)
        total_sum = jnp.zeros((buffer_rows, D), jnp.float32)
        for lane_block in range(N_TP):
            part_sum = jnp.dot(hidden[:, lane_block * half_width:(lane_block + 1) * half_width], down_proj[expert_index, lane_block * half_width:(lane_block + 1) * half_width], preferred_element_type=jnp.float32)
            part_sum = lax.optimization_barrier(part_sum.astype(jnp.bfloat16))
            total_sum = total_sum + part_sum.astype(jnp.float32)
        target_rows = jnp.where(is_valid, picked, route_count).astype(jnp.int32)
        return (total_sum.astype(jnp.bfloat16), target_rows)
    outputs, targets = lax.map(one_expert, jnp.arange(expert_count, dtype=jnp.int32))
    per_route = jnp.zeros((route_count + 1, D), jnp.bfloat16).at[targets.reshape(-1)].set(outputs.reshape(-1, D))[:route_count]
    chosen = per_route.reshape(token_count, TOP, D).astype(jnp.float32)
    group_ids = (route_ids // EXP_GRP).astype(jnp.int32)
    group_part = jnp.take_along_axis(group_weight, group_ids, axis=1)
    gate_values = group_part * expert_weight / lax.optimization_barrier(jnp.sum(expert_weight, axis=1, keepdims=True))
    return lax.optimization_barrier(jnp.sum(chosen * gate_values[:, :, None], axis=1)).astype(jnp.bfloat16)
```

```python
import jax
import jax.numpy as jnp
from jax import lax
from jax.sharding import PartitionSpec as P

TOP = 8
EXP_GRP = 8


EPSILON = 1e-06


def cut_along(array, dim, size):
    lengths = array.shape
    blocks = array.reshape(*lengths[:dim], size, lengths[dim] // size, *lengths[dim + 1 :])
    return jnp.moveaxis(blocks, dim, 0)


def sum_at_owner(array, axis, dim):
    size = lax.axis_size(axis)
    blocks = lax.all_to_all(cut_along(array, dim, size), axis, 0, 0, tiled=True)
    return jnp.sum(blocks.astype(jnp.float32), axis=0)


def on_device(
    tokens_in, norm_gain, gate_proj, up_proj, down_proj, route_ids, group_weight, expert_weight
):
    token_count, model_width = tokens_in.shape
    expert_count = gate_proj.shape[0] * lax.axis_size("ep")
    lane_count = lax.axis_size("tp")
    part_width = model_width // lane_count
    capacity = min(token_count, max(2, 2 * token_count * TOP // expert_count))
    slot_total = expert_count * capacity
    row_values = tokens_in.astype(jnp.float32)
    inv_scale = lax.rsqrt(jnp.mean(row_values * row_values, axis=-1, keepdims=True) + EPSILON)
    normed = (row_values * inv_scale * norm_gain).astype(jnp.bfloat16)
    route_count = token_count * TOP
    flat_ids = route_ids.reshape(route_count)
    positions = jnp.arange(route_count, dtype=jnp.int32)
    same_expert = (flat_ids[:, None] == flat_ids[None, :]) & (
        positions[None, :] < positions[:, None]
    )
    slot_rank = jnp.sum(same_expert.astype(jnp.int32), axis=1)
    slot_index = flat_ids * capacity + slot_rank
    slot_match = jnp.arange(slot_total, dtype=jnp.int32)[:, None] == slot_index[None, :]
    selector = jnp.sum(
        slot_match.reshape(slot_total, token_count, TOP).astype(jnp.int32), axis=2
    ).astype(jnp.bfloat16)
    gate_local = gate_proj[0]
    up_local = up_proj[0]
    lane_index = lax.axis_index("tp")
    own_half = lax.dynamic_slice_in_dim(normed, lane_index * part_width, part_width, 1)
    outgoing = jnp.dot(selector, own_half, preferred_element_type=jnp.float32).astype(jnp.bfloat16)
    arrived = lax.all_to_all(
        outgoing.reshape(expert_count, capacity, part_width),
        "ep",
        split_axis=0,
        concat_axis=0,
        tiled=True,
    )
    arrived = arrived.reshape(slot_total, part_width)
    swap = [(lane, lane_count - 1 - lane) for lane in range(lane_count)]
    partner = lax.ppermute(arrived, "tp", swap)
    column_piece = jnp.where(
        lane_index == 0,
        jnp.concatenate([arrived, partner], axis=1),
        jnp.concatenate([partner, arrived], axis=1),
    )
    gate_acts = jnp.dot(column_piece, gate_local, preferred_element_type=jnp.float32)
    up_acts = jnp.dot(column_piece, up_local, preferred_element_type=jnp.float32)
    hidden = (jax.nn.silu(gate_acts) * up_acts).astype(jnp.bfloat16)
    partial_rows = jnp.dot(hidden, down_proj[0], preferred_element_type=jnp.float32)
    summed = sum_at_owner(
        partial_rows.reshape(expert_count, capacity, model_width).astype(jnp.bfloat16), "tp", 2
    )
    results = summed.astype(jnp.bfloat16)
    returned = lax.all_to_all(results, "ep", split_axis=0, concat_axis=0, tiled=True).reshape(
        slot_total, part_width
    )
    picked = returned[slot_index].astype(jnp.float32).reshape(token_count, TOP, part_width)
    group_ids = route_ids // EXP_GRP
    group_count = group_weight.shape[1]
    group_match = (
        group_ids[:, :, None] == jnp.arange(group_count, dtype=jnp.int32)[None, None, :]
    ).astype(jnp.float32)
    group_part = jnp.sum(group_weight[:, None, :] * group_match, axis=2)
    gate_values = group_part * expert_weight / jnp.sum(expert_weight, axis=1, keepdims=True)
    return jnp.sum(picked * gate_values[:, :, None], axis=1).astype(jnp.bfloat16)


def solution(mesh):
    in_specs = (
        P(("grp", "ep"), None),
        P(),
        P("ep", None, "tp"),
        P("ep", None, "tp"),
        P("ep", "tp", None),
        P(("grp", "ep"), None),
        P(("grp", "ep"), None),
        P(("grp", "ep"), None),
    )
    out_specs = P(("grp", "ep"), "tp")
    return jax.shard_map(
        on_device, mesh=mesh, in_specs=in_specs, out_specs=out_specs, check_vma=False
    )
```

```python
import jax
import jax.numpy as jnp
from jax import lax
from jax.sharding import PartitionSpec as P

TOP = 8
EXP_GRP = 8
LANES = 128

EPSILON = 1e-06
AXES = ("ep", "tp")


def shift_pairs(gathering, delta):
    lanes = lax.axis_size("tp")
    side = EXP_GRP
    pairs = []
    for device in range(lax.axis_size("ep")):
        row, col = divmod(device, side)
        for lane in range(lanes):
            if (lane == 0) == gathering:
                target = ((row + delta) % side) * side + col
            else:
                target = row * side + (col + delta) % side
            pairs.append((device * lanes + lane, target * lanes + lane))
    return pairs


def shift(array, gathering, delta):
    return lax.ppermute(array, AXES, shift_pairs(gathering, delta))


def gather_blocks(block):
    back1 = shift(block, True, 1)
    back7 = shift(block, True, -1)
    back4 = shift(block, True, 4)
    back23 = shift(jnp.stack([block, back1]), True, 2)
    back65 = shift(jnp.stack([block, back7]), True, -2)
    return jnp.stack([block, back1, back23[0], back23[1], back4, back65[1], back65[0], back7])


def scatter_sum(partial):
    low = partial.astype(jnp.bfloat16)
    from2 = shift(jnp.stack([low[2], low[3]]), True, -2).astype(jnp.float32)
    from6 = shift(jnp.stack([low[6], low[5]]), True, 2).astype(jnp.float32)
    from4 = shift(low[4], True, -4).astype(jnp.float32)
    from1 = shift((partial[1] + from2[1]).astype(jnp.bfloat16), True, -1).astype(jnp.float32)
    from7 = shift((partial[7] + from6[1]).astype(jnp.bfloat16), True, 1).astype(jnp.float32)
    return partial[0] + from2[0] + from6[0] + from4 + from1 + from7


def on_device(
    tokens_in, norm_gain, gate_proj, up_proj, down_proj, route_ids, group_weight, expert_weight
):
    token_count, model_width = tokens_in.shape
    expert_count = gate_proj.shape[0] * lax.axis_size("ep")
    lane_count = lax.axis_size("tp")
    part_width = model_width // lane_count
    side = EXP_GRP
    capacity = min(token_count, max(2, 2 * token_count * TOP // expert_count))
    lane_index = lax.axis_index("tp")
    place = lax.axis_index("ep")
    swap = [(lane, lane_count - 1 - lane) for lane in range(lane_count)]

    row_values = tokens_in.astype(jnp.float32)
    inv_scale = lax.rsqrt(jnp.mean(row_values * row_values, axis=-1, keepdims=True) + EPSILON)
    normed = (row_values * inv_scale * norm_gain).astype(jnp.bfloat16)
    own_half = lax.dynamic_slice_in_dim(normed, lane_index * part_width, part_width, 1)

    group_ids = route_ids // EXP_GRP
    group_count = group_weight.shape[1]
    group_match = (
        group_ids[:, :, None] == jnp.arange(group_count, dtype=jnp.int32)[None, None, :]
    ).astype(jnp.float32)
    group_part = jnp.sum(group_weight[:, None, :] * group_match, axis=2)
    gate_values = group_part * expert_weight / jnp.sum(expert_weight, axis=1, keepdims=True)
    high = lax.reduce_precision(gate_values, 8, 7)
    middle = lax.reduce_precision(gate_values - high, 8, 7)
    lowest = gate_values - high - middle
    extra = jnp.concatenate([route_ids.astype(jnp.float32), high, middle, lowest], axis=1)
    extra = jnp.pad(extra, ((0, 0), (0, LANES - extra.shape[1]))).astype(jnp.bfloat16)

    blocks = gather_blocks(jnp.concatenate([own_half, extra], axis=1))
    rows = blocks[:, :, :part_width]
    info = blocks[:, :, part_width : part_width + 4 * TOP].astype(jnp.float32)
    ids = info[:, :, :TOP]
    gates = info[:, :, TOP : 2 * TOP] + info[:, :, 2 * TOP : 3 * TOP] + info[:, :, 3 * TOP :]

    row, col = place // side, place % side
    deltas = jnp.arange(side, dtype=jnp.int32)
    targets = jnp.where(
        lane_index == 0, row * side + (col + deltas) % side, ((row + deltas) % side) * side + col
    ).astype(jnp.float32)
    match = (ids[:, :, None, :] == targets[None, None, :, None]).astype(jnp.float32)
    named = jnp.sum(match, axis=3)
    weight = jnp.sum(match * gates[:, :, None, :], axis=3)
    before = jnp.tril(jnp.ones((token_count, token_count), jnp.bfloat16), -1)
    rank = jnp.einsum(
        "ut,std->sud", before, named.astype(jnp.bfloat16), preferred_element_type=jnp.float32
    )
    slots = jnp.arange(capacity, dtype=jnp.float32)
    chosen = (rank[:, :, :, None] == slots) & (named[:, :, :, None] > 0)
    chosen = chosen.reshape(side, token_count, side * capacity)
    outgoing = lax.dot_general(
        chosen.astype(jnp.bfloat16),
        rows,
        (((1,), (1,)), ((0,), (0,))),
        preferred_element_type=jnp.float32,
    ).astype(jnp.bfloat16)
    outgoing = outgoing.reshape(side, side, capacity, part_width)
    chunk = side * capacity
    arrived = [outgoing[:, 0].reshape(chunk, part_width)] + [
        shift(outgoing[:, delta].reshape(chunk, part_width), False, delta)
        for delta in range(1, side)
    ]
    own_rows = jnp.concatenate(arrived, axis=0)

    def other_order(array):
        blocks = array.reshape(side, side, capacity, array.shape[-1])
        return jnp.swapaxes(blocks, 0, 1).reshape(array.shape)

    partner_rows = other_order(lax.ppermute(own_rows, "tp", swap))

    def project(weights):
        own = lax.dynamic_slice_in_dim(weights, lane_index * part_width, part_width, 0)
        other = lax.dynamic_slice_in_dim(weights, (1 - lane_index) * part_width, part_width, 0)
        return jnp.dot(own_rows, own, preferred_element_type=jnp.float32) + jnp.dot(
            partner_rows, other, preferred_element_type=jnp.float32
        )

    hidden = (jax.nn.silu(project(gate_proj[0])) * project(up_proj[0])).astype(jnp.bfloat16)
    down = down_proj[0]
    own_down = lax.dynamic_slice_in_dim(down, lane_index * part_width, part_width, 1)
    other_down = lax.dynamic_slice_in_dim(down, (1 - lane_index) * part_width, part_width, 1)
    mine = jnp.dot(hidden, own_down, preferred_element_type=jnp.float32).astype(jnp.bfloat16)
    theirs = jnp.dot(
        other_order(hidden), other_down, preferred_element_type=jnp.float32
    ).astype(jnp.bfloat16)
    received = lax.ppermute(theirs, "tp", swap)
    results = (mine.astype(jnp.float32) + received.astype(jnp.float32)).astype(jnp.bfloat16)
    results = results.reshape(side, chunk, part_width)
    returned = [results[0]] + [shift(results[delta], False, -delta) for delta in range(1, side)]
    returned = jnp.stack(returned).reshape(side, side, capacity, part_width)
    returned = jnp.swapaxes(returned, 0, 1).reshape(side, chunk, part_width)
    factors = jnp.where(
        chosen.reshape(side, token_count, side, capacity), weight[:, :, :, None], 0.0
    ).reshape(side, token_count, chunk)
    factors_high = lax.reduce_precision(factors, 8, 7)
    factors_low = (factors - factors_high).astype(jnp.bfloat16)

    def mix(values):
        return lax.dot_general(
            values, returned, (((2,), (1,)), ((0,), (0,))), preferred_element_type=jnp.float32
        )

    return scatter_sum(mix(factors_high.astype(jnp.bfloat16)) + mix(factors_low)).astype(jnp.bfloat16)


def solution(mesh):
    in_specs = (
        P(("grp", "ep"), None),
        P(),
        P("ep", None, "tp"),
        P("ep", None, "tp"),
        P("ep", "tp", None),
        P(("grp", "ep"), None),
        P(("grp", "ep"), None),
        P(("grp", "ep"), None),
    )
    out_specs = P(("grp", "ep"), "tp")
    return jax.shard_map(
        on_device, mesh=mesh, in_specs=in_specs, out_specs=out_specs, check_vma=False
    )
```

```python
import functools

import jax
import jax.numpy as jnp
from jax import lax
from jax.experimental import pallas as pl
from jax.experimental.pallas import tpu as pltpu
from jax.sharding import PartitionSpec as P


TOP = 8
EXP_GRP = 8
LANES = 128

EPSILON = 1e-06
AXES = ("ep", "tp")


def shift_pairs(gathering, delta):
    lanes = lax.axis_size("tp")
    side = EXP_GRP
    pairs = []
    for device in range(lax.axis_size("ep")):
        row, col = divmod(device, side)
        for lane in range(lanes):
            if (lane == 0) == gathering:
                target = ((row + delta) % side) * side + col
            else:
                target = row * side + (col + delta) % side
            pairs.append((device * lanes + lane, target * lanes + lane))
    return pairs


def shift(array, gathering, delta):
    return lax.ppermute(array, AXES, shift_pairs(gathering, delta))


def call(kernel, outputs, *operands, scalars=0, scratch=(), far=False, limit=8):
    smem = pl.BlockSpec(memory_space=pltpu.SMEM)
    vmem = pl.BlockSpec(memory_space=pltpu.VMEM)
    rest = pl.BlockSpec(memory_space=pltpu.HBM) if far else vmem
    return pl.pallas_call(
        kernel,
        out_shape=[jax.ShapeDtypeStruct(*output) for output in outputs],
        in_specs=[smem] * scalars + [rest] * (len(operands) - scalars),
        out_specs=[vmem] * len(outputs),
        scratch_shapes=list(scratch),
        compiler_params=pltpu.CompilerParams(vmem_limit_bytes=limit << 20),
    )(*operands)


def fdot(left, right, contract=((1,), (0,))):
    return lax.dot_general(left, right, (contract, ((), ())), preferred_element_type=jnp.float32)


def prepare_kernel(lane_ref, *refs):
    far, out_ref, near, sems = refs[:5], refs[5], refs[6:11], refs[11]
    copies = [pltpu.make_async_copy(far[n], near[n], sems.at[n]) for n in range(5)]
    for copy in copies:
        copy.start()
    for copy in copies:
        copy.wait()
    tokens_ref, gain_ref, ids_ref, group_ref, expert_ref = near
    half = out_ref.shape[1] - LANES
    width = tokens_ref.shape[1]
    values = tokens_ref[...].astype(jnp.float32)
    mean = jnp.sum(values * values, axis=1, keepdims=True) / width
    scale = lax.rsqrt(mean + EPSILON)
    start = pl.multiple_of(lane_ref[0] * half, half)
    own = tokens_ref[:, pl.ds(start, half)].astype(jnp.float32)
    out_ref[:, :half] = (own * scale * gain_ref[:, pl.ds(start, half)]).astype(jnp.bfloat16)
    ids = ids_ref[...]
    group_ids = lax.div(ids, jnp.full_like(ids, EXP_GRP))
    part = jnp.zeros(ids.shape, jnp.float32)
    for group in range(group_ref.shape[0]):
        part += jnp.where(group_ids == group, group_ref[group : group + 1, :], 0.0)
    weights = expert_ref[...]
    gates = part * weights / jnp.sum(weights, axis=0, keepdims=True)
    high = gates.astype(jnp.bfloat16)
    rest = gates - high.astype(jnp.float32)
    middle = rest.astype(jnp.bfloat16)
    lowest = (rest - middle.astype(jnp.float32)).astype(jnp.bfloat16)
    place = lax.broadcasted_iota(jnp.int32, (TOP, LANES), 0)
    column = lax.broadcasted_iota(jnp.int32, (TOP, LANES), 1)
    packed = jnp.zeros((out_ref.shape[0], LANES), jnp.float32)
    terms = (ids.astype(jnp.float32).astype(jnp.bfloat16), high, middle, lowest)
    for number, term in enumerate(terms):
        spot = (column == place + number * TOP).astype(jnp.float32).astype(jnp.bfloat16)
        packed += fdot(term, spot, ((0,), (0,)))
    out_ref[:, half:] = packed.astype(jnp.bfloat16)


def select_kernel(capacity, targets_ref, *refs):
    side = EXP_GRP
    blocks, outs, factors_ref, held = refs[:side], refs[side : 2 * side], refs[2 * side], refs[-1]
    tokens = blocks[0].shape[0]
    half = outs[0].shape[1]
    for source in range(side):
        held[source] = blocks[source][...]
    lane = lax.broadcasted_iota(jnp.int32, (1, LANES), 1)
    target = jnp.zeros((1, LANES), jnp.int32)
    for number in range(side):
        target = jnp.where(lane // capacity == number, targets_ref[number], target)
    target = target.astype(jnp.float32)
    slot = (lane % capacity).astype(jnp.float32)
    below = lax.broadcasted_iota(jnp.int32, (tokens, tokens), 0)
    above = lax.broadcasted_iota(jnp.int32, (tokens, tokens), 1)
    before = (above < below).astype(jnp.float32).astype(jnp.bfloat16)

    def one_source(source, carry):
        info = held[source, :, half:].astype(jnp.float32)
        gates = (
            info
            + pltpu.roll(info, LANES - TOP, 1)
            + pltpu.roll(info, LANES - 2 * TOP, 1)
        )
        named = jnp.zeros((tokens, LANES), jnp.float32)
        weight = jnp.zeros((tokens, LANES), jnp.float32)
        for choice in range(TOP):
            same = info[:, choice : choice + 1] == target
            named = jnp.where(same, 1.0, named)
            weight = jnp.where(same, gates[:, TOP + choice : TOP + choice + 1], weight)
        rank = fdot(before, named.astype(jnp.bfloat16))
        chosen = jnp.where(rank == slot, named, 0.0)
        factors = chosen * weight
        high = factors.astype(jnp.bfloat16)
        factors_ref[source, :tokens] = high
        factors_ref[source, tokens:] = (factors - high.astype(jnp.float32)).astype(jnp.bfloat16)
        rows = fdot(chosen.astype(jnp.bfloat16), held[source, :, :half], ((0,), (0,)))
        rows = rows.astype(jnp.bfloat16)
        spot = pl.ds(pl.multiple_of(source * capacity, capacity), capacity)
        for number in range(side):
            outs[number][spot, :] = rows[number * capacity : (number + 1) * capacity, :]
        return carry

    lax.fori_loop(0, side, one_source, 0)


def project(chunks, weights, start, out_ref, begin):
    chunk, half = chunks[0].shape
    hidden = weights[0].shape[1]
    for first in range(0, len(chunks), 2):
        rows = jnp.concatenate([chunks[first][...], chunks[first + 1][...]], axis=0)
        for number, weight_ref in enumerate(weights):
            out_ref[
                begin + first * chunk : begin + (first + 2) * chunk,
                number * hidden : (number + 1) * hidden,
            ] = fdot(rows, weight_ref[pl.ds(start, half), :])


def early_kernel(lane_ref, *refs):
    number = (len(refs) - 4) // 2
    own, partner = refs[:number], refs[number : 2 * number]
    weights, own_out, partner_out = refs[2 * number : -2], refs[-2], refs[-1]
    half = own[0].shape[1]
    project(own, weights, pl.multiple_of(lane_ref[0] * half, half), own_out, 0)
    project(partner, weights, pl.multiple_of((1 - lane_ref[0]) * half, half), partner_out, 0)


def late_kernel(capacity, lane_ref, *refs):
    side = EXP_GRP
    number = side // 2
    own, partner = refs[:number], refs[number : 2 * number]
    weights, own_early, partner_early = refs[2 * number : -6], refs[-6], refs[-5]
    mine_ref, theirs_ref, own_late, partner_late = refs[-4:]
    chunk, half = own[0].shape
    hidden = mine_ref.shape[1]
    project(own, weights, pl.multiple_of(lane_ref[0] * half, half), own_late, 0)
    project(partner, weights, pl.multiple_of((1 - lane_ref[0]) * half, half), partner_late, 0)

    def block(index, first, second, owned, partnered):
        one, two = index // number, index % number
        left = pl.multiple_of(one * chunk + (second * number + two) * capacity, capacity)
        right = pl.multiple_of(two * chunk + (first * number + one) * capacity, capacity)
        both = owned[pl.ds(left, capacity), :] + partnered[pl.ds(right, capacity), :]
        gate, up = both[:, :hidden], both[:, hidden:]
        acts = (gate / (1.0 + jnp.exp(-gate)) * up).astype(jnp.bfloat16)
        far = number * chunk
        mine_ref[pl.ds(pl.multiple_of(first * far + left, capacity), capacity), :] = acts
        theirs_ref[pl.ds(pl.multiple_of(second * far + right, capacity), capacity), :] = acts

    def blocks(index, carry):
        for first, owned in ((0, own_early), (1, own_late)):
            for second, partnered in ((0, partner_early), (1, partner_late)):
                block(index, first, second, owned, partnered)
        return carry

    lax.fori_loop(0, number * number, blocks, 0)


def down_kernel(places, lane_ref, mine_ref, received_ref, down_ref, other_ref, *outs):
    chunk, half = outs[0].shape
    start = pl.multiple_of(lane_ref[0] * half, half)
    for place, out_ref in zip(places, outs):
        begin = place * chunk
        out_ref[...] = (
            fdot(mine_ref[begin : begin + chunk, :], down_ref[:, pl.ds(start, half)])
            + fdot(received_ref[begin : begin + chunk, :], other_ref[:, pl.ds(start, half)])
        ).astype(jnp.bfloat16)


def combine_kernel(capacity, *refs):
    side = EXP_GRP
    chunks, factors_ref, outs = refs[:side], refs[side], refs[side + 1 :]
    for source in range(side):
        rows = jnp.concatenate(
            [chunk[source * capacity : (source + 1) * capacity, :] for chunk in chunks], axis=0
        )
        both = fdot(factors_ref[source], rows)
        tokens = both.shape[0] // 2
        outs[source][...] = (both[:tokens] + both[tokens:]).astype(outs[source].dtype)


def layer(
    tokens_in, norm_gain, gate_proj, up_proj, down_proj, route_ids, group_weight, expert_weight
):
    token_count, model_width = tokens_in.shape
    expert_count = gate_proj.shape[0] * lax.axis_size("ep")
    lane_count = lax.axis_size("tp")
    part_width = model_width // lane_count
    hidden_width = gate_proj.shape[2]
    side = EXP_GRP
    capacity = min(token_count, max(2, 2 * token_count * TOP // expert_count))
    chunk = side * capacity
    order = (0, 4, 3, 5, 2, 6, 1, 7)
    lane_index = lax.axis_index("tp")
    lane = lane_index.reshape(1)
    place = lax.axis_index("ep")
    row, col = place // side, place % side
    deltas = jnp.asarray(order, jnp.int32)
    targets = jnp.where(
        lane_index == 0, row * side + (col + deltas) % side, ((row + deltas) % side) * side + col
    )
    swap = [(number, lane_count - 1 - number) for number in range(lane_count)]
    half_type = jnp.bfloat16

    other_down = lax.ppermute(down_proj[0], "tp", swap)
    (packed,) = call(
        prepare_kernel,
        [((token_count, part_width + LANES), half_type)],
        lane,
        tokens_in,
        norm_gain.reshape(1, model_width),
        route_ids.T,
        group_weight.T,
        expert_weight.T,
        scalars=1,
        far=True,
        scratch=[
            pltpu.VMEM((token_count, model_width), half_type),
            pltpu.VMEM((1, model_width), jnp.float32),
            pltpu.VMEM((TOP, token_count), jnp.int32),
            pltpu.VMEM((group_weight.shape[1], token_count), jnp.float32),
            pltpu.VMEM((TOP, token_count), jnp.float32),
            pltpu.SemaphoreType.DMA((5,)),
        ],
    )
    blocks = [packed]
    for delta in order[1:]:
        blocks.append(shift(packed, True, delta))
    *outgoing, factors = call(
        functools.partial(select_kernel, capacity),
        [((chunk, part_width), half_type)] * side
        + [((side, 2 * token_count, chunk), half_type)],
        targets,
        *blocks,
        scalars=1,
        scratch=[pltpu.VMEM((side,) + packed.shape, half_type)],
    )
    own = [outgoing[0]]
    for place, delta in enumerate(order[1:], 1):
        own.append(shift(outgoing[place], False, delta))
    partner = [lax.ppermute(rows, "tp", swap) for rows in own]
    number = side // 2
    weights = (gate_proj[0], up_proj[0])
    sums = ((number * chunk, 2 * hidden_width), jnp.float32)
    early = call(
        early_kernel, [sums] * 2, lane, *own[:number], *partner[:number], *weights, scalars=1
    )
    mine, theirs = call(
        functools.partial(late_kernel, capacity),
        [((side * chunk, hidden_width), half_type)] * 2,
        lane,
        *own[number:],
        *partner[number:],
        *weights,
        *early,
        scalars=1,
        scratch=[pltpu.VMEM(*sums)] * 2,
        limit=16,
    )
    received = lax.ppermute(theirs, "tp", swap)
    returned = [None] * side
    for some in ((1, 2, 3), (4, 5, 6, 7, 0)):
        results = call(
            functools.partial(down_kernel, some),
            [((chunk, part_width), half_type)] * len(some),
            lane,
            mine,
            received,
            down_proj[0],
            other_down,
            scalars=1,
        )
        for place, result in zip(some, results):
            returned[place] = shift(result, False, -order[place]) if place else result
    kept, *partials = call(
        functools.partial(combine_kernel, capacity),
        [((token_count, part_width), jnp.float32)]
        + [((token_count, part_width), half_type)] * (side - 1),
        *returned,
        factors,
    )
    total = kept
    for place, delta in enumerate(order[1:]):
        total += shift(partials[place], True, -delta).astype(jnp.float32)
    return total.astype(half_type)


def solution(mesh):
    in_specs = (
        P(("grp", "ep"), None),
        P(),
        P("ep", None, "tp"),
        P("ep", None, "tp"),
        P("ep", "tp", None),
        P(("grp", "ep"), None),
        P(("grp", "ep"), None),
        P(("grp", "ep"), None),
    )
    out_specs = P(("grp", "ep"), "tp")
    return jax.shard_map(layer, mesh=mesh, in_specs=in_specs, out_specs=out_specs, check_vma=False)
```

```python
import functools

import jax
import jax.numpy as jnp
from jax import lax
from jax.experimental import pallas as pl
from jax.experimental.pallas import tpu as pltpu
from jax.sharding import PartitionSpec as P


TOP = 8
EXP_GRP = 8
LANES = 128

EPSILON = 1e-06
AXES = ("ep", "tp")
ORDER = (0, 4, 3, 5, 2, 6, 1, 7)
EARLY = 4


def shift_pairs(gathering, delta):
    lanes = lax.axis_size("tp")
    side = EXP_GRP
    pairs = []
    for device in range(lax.axis_size("ep")):
        row, col = divmod(device, side)
        for lane in range(lanes):
            if (lane == 0) == gathering:
                target = ((row + delta) % side) * side + col
            else:
                target = row * side + (col + delta) % side
            pairs.append((device * lanes + lane, target * lanes + lane))
    return pairs


def shift(array, gathering, delta):
    return lax.ppermute(array, AXES, shift_pairs(gathering, delta))


def call(kernel, outputs, *operands, scalars=0, scratch=(), far=0, limit=8):
    smem = pl.BlockSpec(memory_space=pltpu.SMEM)
    vmem = pl.BlockSpec(memory_space=pltpu.VMEM)
    hbm = pl.BlockSpec(memory_space=pltpu.HBM)
    near = len(operands) - far
    operands = operands[:near] + tuple(
        pltpu.with_memory_space_constraint(operand, pltpu.HBM) for operand in operands[near:]
    )
    return pl.pallas_call(
        kernel,
        out_shape=[jax.ShapeDtypeStruct(*output) for output in outputs],
        in_specs=[smem] * scalars + [vmem] * (near - scalars) + [hbm] * far,
        out_specs=[vmem] * len(outputs),
        scratch_shapes=list(scratch),
        compiler_params=pltpu.CompilerParams(vmem_limit_bytes=limit << 20),
    )(*operands)


def fdot(left, right, contract=((1,), (0,))):
    return lax.dot_general(left, right, (contract, ((), ())), preferred_element_type=jnp.float32)


def prepare_kernel(lane_ref, *refs):
    far, out_ref, near, sems = refs[:5], refs[5], refs[6:11], refs[11]
    copies = [pltpu.make_async_copy(far[n], near[n], sems.at[n]) for n in range(5)]
    for copy in copies:
        copy.start()
    for copy in copies:
        copy.wait()
    tokens_ref, gain_ref, ids_ref, group_ref, expert_ref = near
    half = out_ref.shape[1]
    count, width = tokens_ref.shape
    values = tokens_ref[...].astype(jnp.float32)
    mean = jnp.sum(values * values, axis=1, keepdims=True) / width
    scale = lax.rsqrt(mean + EPSILON)
    start = pl.multiple_of(lane_ref[0] * half, half)
    own = tokens_ref[:, pl.ds(start, half)].astype(jnp.float32)
    out_ref[:count, :] = (own * scale * gain_ref[:, pl.ds(start, half)]).astype(jnp.bfloat16)
    ids = ids_ref[...]
    group_ids = lax.div(ids, jnp.full_like(ids, EXP_GRP))
    part = jnp.zeros(ids.shape, jnp.float32)
    for group in range(group_ref.shape[0]):
        part += jnp.where(group_ids == group, group_ref[group : group + 1, :], 0.0)
    weights = expert_ref[...]
    gates = part * weights / jnp.sum(weights, axis=0, keepdims=True)
    high = gates.astype(jnp.bfloat16)
    rest = gates - high.astype(jnp.float32)
    middle = rest.astype(jnp.bfloat16)
    lowest = (rest - middle.astype(jnp.float32)).astype(jnp.bfloat16)
    out_ref[count:, :] = jnp.zeros((TOP, half), jnp.bfloat16)
    for number, term in enumerate((ids.astype(jnp.float32).astype(jnp.bfloat16), high, middle, lowest)):
        out_ref[count:, number * LANES : number * LANES + count] = term


def chosen_slots(order, lane_ref, place_ref, blocks):
    side = EXP_GRP
    tokens = blocks[0].shape[0] - TOP
    lane, place = lane_ref[0], place_ref[0]
    row, col = lax.div(place, side), lax.rem(place, side)
    line = lax.broadcasted_iota(jnp.int32, (side, tokens), 0)
    target = jnp.zeros((side, tokens), jnp.int32)
    for number, delta in enumerate(order):
        along = row * side + lax.rem(col + delta, side)
        across = lax.rem(row + delta, side) * side + col
        target = jnp.where(line == number, (1 - lane) * along + lane * across, target)
    target = target.astype(jnp.float32)
    named, gates = [], []
    for source in range(side):
        info = blocks[source][tokens:, : 4 * LANES].astype(jnp.float32)
        ids = info[:, :tokens]
        terms = [info[:, n * LANES : n * LANES + tokens] for n in range(1, 4)]
        weights = terms[0] + terms[1] + terms[2]
        match = jnp.zeros((side, tokens), jnp.float32)
        gate = jnp.zeros((side, tokens), jnp.float32)
        for choice in range(TOP):
            same = ids[choice : choice + 1, :] == target
            match = jnp.where(same, 1.0, match)
            gate = jnp.where(same, weights[choice : choice + 1, :], gate)
        named.append(match)
        gates.append(gate)
    named = jnp.concatenate(named, axis=0)
    first = lax.broadcasted_iota(jnp.int32, (tokens, tokens), 0)
    second = lax.broadcasted_iota(jnp.int32, (tokens, tokens), 1)
    before = (first < second).astype(jnp.float32).astype(jnp.bfloat16)
    rank = fdot(named.astype(jnp.bfloat16), before)
    return jnp.where(named > 0.0, rank, -1.0), gates


def select_kernel(capacity, order, lane_ref, place_ref, *refs):
    side = EXP_GRP
    blocks, outs = refs[:side], refs[side:]
    tokens = blocks[0].shape[0] - TOP
    slots, _ = chosen_slots(order, lane_ref, place_ref, blocks)
    slot = lax.broadcasted_iota(jnp.int32, (capacity, tokens), 0).astype(jnp.float32)
    for source in range(side):
        lines = [slots[source * side + n : source * side + n + 1, :] for n in range(side)]
        chosen = jnp.concatenate([(line == slot).astype(jnp.float32) for line in lines], axis=0)
        rows = fdot(chosen.astype(jnp.bfloat16), blocks[source][:tokens, :]).astype(jnp.bfloat16)
        for number in range(side):
            outs[number][source * capacity : (source + 1) * capacity, :] = rows[
                number * capacity : (number + 1) * capacity, :
            ]


def factors_kernel(capacity, order, lane_ref, place_ref, *refs):
    side = EXP_GRP
    blocks, weights = refs[:side], refs[side : side + 2]
    out_ref, held, sems = refs[side + 2], refs[side + 3 : side + 5], refs[side + 5]
    copies = [pltpu.make_async_copy(weights[n], held[n], sems.at[n]) for n in range(2)]
    for copy in copies:
        copy.start()
    tokens = blocks[0].shape[0] - TOP
    slots, gates = chosen_slots(order, lane_ref, place_ref, blocks)
    slot = lax.broadcasted_iota(jnp.int32, (capacity, tokens), 0).astype(jnp.float32)
    for source in range(side):
        factors = jnp.concatenate(
            [
                jnp.where(
                    slots[source * side + n : source * side + n + 1, :] == slot,
                    gates[source][n : n + 1, :],
                    0.0,
                )
                for n in range(side)
            ],
            axis=0,
        ).T
        high = factors.astype(jnp.bfloat16)
        out_ref[source, :tokens] = high
        out_ref[source, tokens:] = (factors - high.astype(jnp.float32)).astype(jnp.bfloat16)
    for copy in copies:
        copy.wait()


def project(chunks, weights, start, out_ref, begin):
    chunk, half = chunks[0].shape
    hidden = weights[0].shape[1]
    for first in range(0, len(chunks), 2):
        pair = chunks[first : first + 2]
        rows = jnp.concatenate([part[...] for part in pair], axis=0)
        for number, weight_ref in enumerate(weights):
            out_ref[
                begin + first * chunk : begin + (first + len(pair)) * chunk,
                number * hidden : (number + 1) * hidden,
            ] = fdot(rows, weight_ref[pl.ds(start, half), :])


def early_kernel(lane_ref, *refs):
    own, partner = refs[:EARLY], refs[EARLY : 2 * EARLY]
    weights, own_out, partner_out = refs[2 * EARLY : -2], refs[-2], refs[-1]
    half = own[0].shape[1]
    project(own, weights, pl.multiple_of(lane_ref[0] * half, half), own_out, 0)
    project(partner, weights, pl.multiple_of((1 - lane_ref[0]) * half, half), partner_out, 0)


def late_kernel(capacity, lane_ref, *refs):
    side = EXP_GRP
    late = side - EARLY
    own, partner = refs[:late], refs[late : 2 * late]
    weights, own_early, partner_early = refs[2 * late : -7], refs[-7], refs[-6]
    mine_ref, own_late, partner_late = refs[-5], refs[-2], refs[-1]
    theirs_refs = refs[-4:-2]
    chunk, half = own[0].shape
    hidden = mine_ref.shape[1]
    project(own, weights, pl.multiple_of(lane_ref[0] * half, half), own_late, 0)
    project(partner, weights, pl.multiple_of((1 - lane_ref[0]) * half, half), partner_late, 0)
    rows = ((0, EARLY, own_early), (EARLY, late, own_late))
    cols = ((0, EARLY, partner_early, theirs_refs[0]), (EARLY, late, partner_late, theirs_refs[1]))
    for base, count, owned in rows:
        for far_base, far_count, partnered, theirs_ref in cols:

            def block(index, carry):
                one = lax.div(index, far_count)
                two = index - one * far_count
                left = pl.multiple_of(one * chunk + (far_base + two) * capacity, capacity)
                right = pl.multiple_of(two * chunk + (base + one) * capacity, capacity)
                both = owned[pl.ds(left, capacity), :] + partnered[pl.ds(right, capacity), :]
                gate, up = both[:, :hidden], both[:, hidden:]
                acts = (gate / (1.0 + jnp.exp(-gate)) * up).astype(jnp.bfloat16)
                whole = pl.multiple_of(base * chunk + left, capacity)
                mine_ref[pl.ds(whole, capacity), :] = acts
                theirs_ref[pl.ds(right, capacity), :] = acts
                return carry

            lax.fori_loop(0, count * far_count, block, 0, unroll=2)


def down_kernel(places, lane_ref, mine_ref, near_ref, far_ref, down_ref, other_ref, *outs):
    chunk, half = outs[0].shape
    start = pl.multiple_of(lane_ref[0] * half, half)
    for place, out_ref in zip(places, outs):
        begin = place * chunk
        received_ref = far_ref if place >= EARLY else near_ref
        at = begin - EARLY * chunk if place >= EARLY else begin
        out_ref[...] = (
            fdot(mine_ref[begin : begin + chunk, :], down_ref[:, pl.ds(start, half)])
            + fdot(received_ref[at : at + chunk, :], other_ref[:, pl.ds(start, half)])
        ).astype(jnp.bfloat16)


def combine_kernel(capacity, *refs):
    side = EXP_GRP
    chunks, factors_ref, outs = refs[:side], refs[side], refs[side + 1 :]
    for source in range(side):
        rows = jnp.concatenate(
            [chunk[source * capacity : (source + 1) * capacity, :] for chunk in chunks], axis=0
        )
        both = fdot(factors_ref[source], rows)
        tokens = both.shape[0] // 2
        outs[source][...] = (both[:tokens] + both[tokens:]).astype(outs[source].dtype)


def layer(
    tokens_in, norm_gain, gate_proj, up_proj, down_proj, route_ids, group_weight, expert_weight
):
    token_count, model_width = tokens_in.shape
    expert_count = gate_proj.shape[0] * lax.axis_size("ep")
    lane_count = lax.axis_size("tp")
    part_width = model_width // lane_count
    hidden_width = gate_proj.shape[2]
    side = EXP_GRP
    capacity = min(token_count, max(2, 2 * token_count * TOP // expert_count))
    chunk = side * capacity
    order = ORDER
    lane_index = lax.axis_index("tp")
    lane = lane_index.reshape(1)
    place = lax.axis_index("ep")
    spot = place.reshape(1)
    swap = [(number, lane_count - 1 - number) for number in range(lane_count)]
    half_type = jnp.bfloat16

    other_down = lax.ppermute(down_proj[0], "tp", swap)
    (packed,) = call(
        prepare_kernel,
        [((token_count + TOP, part_width), half_type)],
        lane,
        tokens_in,
        norm_gain.reshape(1, model_width),
        route_ids.T,
        group_weight.T,
        expert_weight.T,
        scalars=1,
        far=5,
        scratch=[
            pltpu.VMEM((token_count, model_width), half_type),
            pltpu.VMEM((1, model_width), jnp.float32),
            pltpu.VMEM((TOP, token_count), jnp.int32),
            pltpu.VMEM((group_weight.shape[1], token_count), jnp.float32),
            pltpu.VMEM((TOP, token_count), jnp.float32),
            pltpu.SemaphoreType.DMA((5,)),
        ],
    )
    blocks = [packed]
    for delta in order[1:]:
        blocks.append(shift(packed, True, delta))
    outgoing = call(
        functools.partial(select_kernel, capacity, order),
        [((chunk, part_width), half_type)] * side,
        lane,
        spot,
        *blocks,
        scalars=2,
    )
    factors, *weights = call(
        functools.partial(factors_kernel, capacity, order),
        [((side, 2 * token_count, chunk), half_type)]
        + [((model_width, hidden_width), half_type)] * 2,
        lane,
        spot,
        *blocks,
        gate_proj[0],
        up_proj[0],
        scalars=2,
        scratch=[pltpu.SemaphoreType.DMA((2,))],
        far=2,
    )
    own = [outgoing[0]]
    for place, delta in enumerate(order[1:], 1):
        own.append(shift(outgoing[place], False, delta))
    partner = []
    for delta, rows in zip(order, own):
        partner.append(lax.ppermute(rows, "tp", swap))
    sums = ((EARLY * chunk, 2 * hidden_width), jnp.float32)
    early = call(
        early_kernel, [sums] * 2, lane, *own[:EARLY], *partner[:EARLY], *weights, scalars=1
    )
    late = side - EARLY
    mine, *theirs = call(
        functools.partial(late_kernel, capacity),
        [
            ((side * chunk, hidden_width), half_type),
            ((EARLY * chunk, hidden_width), half_type),
            ((late * chunk, hidden_width), half_type),
        ],
        lane,
        *own[EARLY:],
        *partner[EARLY:],
        *weights,
        *early,
        scalars=1,
        scratch=[pltpu.VMEM((late * chunk, 2 * hidden_width), jnp.float32)] * 2,
        limit=16,
    )
    near = lax.ppermute(theirs[0], "tp", swap)
    far = lax.ppermute(theirs[1], "tp", swap)
    returned = [None] * side
    for some in (tuple(range(1, EARLY)), tuple(range(EARLY, side)) + (0,)):
        results = call(
            functools.partial(down_kernel, some),
            [((chunk, part_width), half_type)] * len(some),
            lane,
            mine,
            near,
            far if some[0] >= EARLY else near,
            down_proj[0],
            other_down,
            scalars=1,
        )
        for place, result in zip(some, results):
            returned[place] = shift(result, False, -order[place]) if place else result
    kept, *partials = call(
        functools.partial(combine_kernel, capacity),
        [((token_count, part_width), jnp.float32)]
        + [((token_count, part_width), half_type)] * (side - 1),
        *returned,
        factors,
    )
    total = kept
    for place, delta in enumerate(order[1:]):
        total += shift(partials[place], True, -delta).astype(jnp.float32)
    return total.astype(half_type)


def solution(mesh):
    in_specs = (
        P(("grp", "ep"), None),
        P(),
        P("ep", None, "tp"),
        P("ep", None, "tp"),
        P("ep", "tp", None),
        P(("grp", "ep"), None),
        P(("grp", "ep"), None),
        P(("grp", "ep"), None),
    )
    out_specs = P(("grp", "ep"), "tp")
    return jax.shard_map(layer, mesh=mesh, in_specs=in_specs, out_specs=out_specs, check_vma=False)
```

```python
import functools

import jax
import jax.numpy as jnp
from jax import lax
from jax.experimental import pallas as pl
from jax.experimental.pallas import tpu as pltpu
from jax.sharding import PartitionSpec as P


TOP = 8
EXP_GRP = 8
LANES = 128

EPSILON = 1e-06
AXES = ("ep", "tp")
ORDER = (0, 4, 3, 5, 2, 6, 1, 7)
EARLY = 4


def shift_pairs(gathering, delta):
    lanes = lax.axis_size("tp")
    side = EXP_GRP
    pairs = []
    for device in range(lax.axis_size("ep")):
        row, col = divmod(device, side)
        for lane in range(lanes):
            if (lane == 0) == gathering:
                target = ((row + delta) % side) * side + col
            else:
                target = row * side + (col + delta) % side
            pairs.append((device * lanes + lane, target * lanes + lane))
    return pairs


def shift(array, gathering, delta):
    return lax.ppermute(array, AXES, shift_pairs(gathering, delta))


def call(kernel, outputs, *operands, scalars=0, scratch=(), far=0, limit=8):
    smem = pl.BlockSpec(memory_space=pltpu.SMEM)
    vmem = pl.BlockSpec(memory_space=pltpu.VMEM)
    hbm = pl.BlockSpec(memory_space=pltpu.HBM)
    near = len(operands) - far
    operands = operands[:near] + tuple(
        pltpu.with_memory_space_constraint(operand, pltpu.HBM) for operand in operands[near:]
    )
    return pl.pallas_call(
        kernel,
        out_shape=[jax.ShapeDtypeStruct(*output) for output in outputs],
        in_specs=[smem] * scalars + [vmem] * (near - scalars) + [hbm] * far,
        out_specs=[vmem] * len(outputs),
        scratch_shapes=list(scratch),
        compiler_params=pltpu.CompilerParams(vmem_limit_bytes=limit << 20),
    )(*operands)


def fdot(left, right, contract=((1,), (0,))):
    return lax.dot_general(left, right, (contract, ((), ())), preferred_element_type=jnp.float32)


def prepare_kernel(lane_ref, *refs):
    far, out_ref, near, sems = refs[:5], refs[5], refs[6:11], refs[11]
    copies = [pltpu.make_async_copy(far[n], near[n], sems.at[n]) for n in range(5)]
    for copy in copies:
        copy.start()
    for copy in copies:
        copy.wait()
    tokens_ref, gain_ref, ids_ref, group_ref, expert_ref = near
    half = out_ref.shape[1]
    count, width = tokens_ref.shape
    values = tokens_ref[...].astype(jnp.float32)
    mean = jnp.sum(values * values, axis=1, keepdims=True) / width
    scale = lax.rsqrt(mean + EPSILON)
    start = pl.multiple_of(lane_ref[0] * half, half)
    own = tokens_ref[:, pl.ds(start, half)].astype(jnp.float32)
    out_ref[:count, :] = (own * scale * gain_ref[:, pl.ds(start, half)]).astype(jnp.bfloat16)
    ids = ids_ref[...]
    group_ids = lax.div(ids, jnp.full_like(ids, EXP_GRP))
    part = jnp.zeros(ids.shape, jnp.float32)
    for group in range(group_ref.shape[0]):
        part += jnp.where(group_ids == group, group_ref[group : group + 1, :], 0.0)
    weights = expert_ref[...]
    gates = part * weights / jnp.sum(weights, axis=0, keepdims=True)
    high = gates.astype(jnp.bfloat16)
    rest = gates - high.astype(jnp.float32)
    middle = rest.astype(jnp.bfloat16)
    lowest = (rest - middle.astype(jnp.float32)).astype(jnp.bfloat16)
    out_ref[count:, :] = jnp.zeros((TOP, half), jnp.bfloat16)
    for number, term in enumerate((ids.astype(jnp.float32).astype(jnp.bfloat16), high, middle, lowest)):
        out_ref[count:, number * LANES : number * LANES + count] = term


def chosen_slots(order, lane_ref, place_ref, blocks):
    side = EXP_GRP
    tokens = blocks[0].shape[0] - TOP
    lane, place = lane_ref[0], place_ref[0]
    row, col = lax.div(place, side), lax.rem(place, side)
    line = lax.broadcasted_iota(jnp.int32, (side, tokens), 0)
    target = jnp.zeros((side, tokens), jnp.int32)
    for number, delta in enumerate(order):
        along = row * side + lax.rem(col + delta, side)
        across = lax.rem(row + delta, side) * side + col
        target = jnp.where(line == number, (1 - lane) * along + lane * across, target)
    target = target.astype(jnp.float32)
    named, gates = [], []
    for source in range(side):
        info = blocks[source][tokens:, : 4 * LANES].astype(jnp.float32)
        ids = info[:, :tokens]
        terms = [info[:, n * LANES : n * LANES + tokens] for n in range(1, 4)]
        weights = terms[0] + terms[1] + terms[2]
        match = jnp.zeros((side, tokens), jnp.float32)
        gate = jnp.zeros((side, tokens), jnp.float32)
        for choice in range(TOP):
            same = ids[choice : choice + 1, :] == target
            match = jnp.where(same, 1.0, match)
            gate = jnp.where(same, weights[choice : choice + 1, :], gate)
        named.append(match)
        gates.append(gate)
    named = jnp.concatenate(named, axis=0)
    first = lax.broadcasted_iota(jnp.int32, (tokens, tokens), 0)
    second = lax.broadcasted_iota(jnp.int32, (tokens, tokens), 1)
    before = (first < second).astype(jnp.float32).astype(jnp.bfloat16)
    rank = fdot(named.astype(jnp.bfloat16), before)
    return jnp.where(named > 0.0, rank, -1.0), gates


def select_kernel(capacity, order, lane_ref, place_ref, *refs):
    side = EXP_GRP
    blocks, outs = refs[:side], refs[side:]
    tokens = blocks[0].shape[0] - TOP
    slots, _ = chosen_slots(order, lane_ref, place_ref, blocks)
    slot = lax.broadcasted_iota(jnp.int32, (capacity, tokens), 0).astype(jnp.float32)
    for source in range(side):
        lines = [slots[source * side + n : source * side + n + 1, :] for n in range(side)]
        chosen = jnp.concatenate([(line == slot).astype(jnp.float32) for line in lines], axis=0)
        rows = fdot(chosen.astype(jnp.bfloat16), blocks[source][:tokens, :]).astype(jnp.bfloat16)
        for number in range(side):
            outs[number][source * capacity : (source + 1) * capacity, :] = rows[
                number * capacity : (number + 1) * capacity, :
            ]


def factors_kernel(capacity, order, lane_ref, place_ref, *refs):
    side = EXP_GRP
    blocks, weights = refs[:side], refs[side : side + 2]
    out_ref, held, sems = refs[side + 2], refs[side + 3 : side + 5], refs[side + 5]
    copies = [pltpu.make_async_copy(weights[n], held[n], sems.at[n]) for n in range(2)]
    for copy in copies:
        copy.start()
    tokens = blocks[0].shape[0] - TOP
    slots, gates = chosen_slots(order, lane_ref, place_ref, blocks)
    slot = lax.broadcasted_iota(jnp.int32, (capacity, tokens), 0).astype(jnp.float32)
    for source in range(side):
        factors = jnp.concatenate(
            [
                jnp.where(
                    slots[source * side + n : source * side + n + 1, :] == slot,
                    gates[source][n : n + 1, :],
                    0.0,
                )
                for n in range(side)
            ],
            axis=0,
        ).T
        high = factors.astype(jnp.bfloat16)
        out_ref[source, :tokens] = high
        out_ref[source, tokens:] = (factors - high.astype(jnp.float32)).astype(jnp.bfloat16)
    for copy in copies:
        copy.wait()


def project(chunks, weights, start, out_ref, begin):
    chunk, half = chunks[0].shape
    hidden = weights[0].shape[1]
    for first in range(0, len(chunks), 2):
        pair = chunks[first : first + 2]
        rows = jnp.concatenate([part[...] for part in pair], axis=0)
        for number, weight_ref in enumerate(weights):
            out_ref[
                begin + first * chunk : begin + (first + len(pair)) * chunk,
                number * hidden : (number + 1) * hidden,
            ] = fdot(rows, weight_ref[pl.ds(start, half), :])


def half_kernel(partner, lane_ref, *refs):
    chunks, weights, out_ref = refs[:-3], refs[-3:-1], refs[-1]
    half = chunks[0].shape[1]
    lane = 1 - lane_ref[0] if partner else lane_ref[0]
    project(chunks, weights, pl.multiple_of(lane * half, half), out_ref, 0)


def late_kernel(capacity, lane_ref, *refs):
    side = EXP_GRP
    late = side - EARLY
    partner, weights = refs[:late], refs[late : late + 2]
    own_early, partner_early, own_late, mine_ref = refs[late + 2 : late + 6]
    theirs_refs, partner_late = refs[late + 6 : late + 8], refs[late + 8]
    chunk, half = partner[0].shape
    hidden = mine_ref.shape[1]
    project(partner, weights, pl.multiple_of((1 - lane_ref[0]) * half, half), partner_late, 0)
    rows = ((0, EARLY, own_early), (EARLY, late, own_late))
    cols = ((0, EARLY, partner_early, theirs_refs[0]), (EARLY, late, partner_late, theirs_refs[1]))
    for base, count, owned in rows:
        for far_base, far_count, partnered, theirs_ref in cols:

            def block(index, carry):
                one = lax.div(index, far_count)
                two = index - one * far_count
                left = pl.multiple_of(one * chunk + (far_base + two) * capacity, capacity)
                right = pl.multiple_of(two * chunk + (base + one) * capacity, capacity)
                both = owned[pl.ds(left, capacity), :] + partnered[pl.ds(right, capacity), :]
                gate, up = both[:, :hidden], both[:, hidden:]
                acts = (gate / (1.0 + jnp.exp(-gate)) * up).astype(jnp.bfloat16)
                whole = pl.multiple_of(base * chunk + left, capacity)
                mine_ref[pl.ds(whole, capacity), :] = acts
                theirs_ref[pl.ds(right, capacity), :] = acts
                return carry

            lax.fori_loop(0, count * far_count, block, 0, unroll=2)


def down_kernel(places, lane_ref, mine_ref, near_ref, far_ref, down_ref, other_ref, *outs):
    chunk, half = outs[0].shape
    start = pl.multiple_of(lane_ref[0] * half, half)
    for place, out_ref in zip(places, outs):
        begin = place * chunk
        received_ref = far_ref if place >= EARLY else near_ref
        at = begin - EARLY * chunk if place >= EARLY else begin
        out_ref[...] = (
            fdot(mine_ref[begin : begin + chunk, :], down_ref[:, pl.ds(start, half)])
            + fdot(received_ref[at : at + chunk, :], other_ref[:, pl.ds(start, half)])
        ).astype(jnp.bfloat16)


def combine_kernel(capacity, *refs):
    side = EXP_GRP
    chunks, factors_ref, outs = refs[:side], refs[side], refs[side + 1 :]
    for source in range(side):
        rows = jnp.concatenate(
            [chunk[source * capacity : (source + 1) * capacity, :] for chunk in chunks], axis=0
        )
        both = fdot(factors_ref[source], rows)
        tokens = both.shape[0] // 2
        outs[source][...] = (both[:tokens] + both[tokens:]).astype(outs[source].dtype)


def layer(
    tokens_in, norm_gain, gate_proj, up_proj, down_proj, route_ids, group_weight, expert_weight
):
    token_count, model_width = tokens_in.shape
    expert_count = gate_proj.shape[0] * lax.axis_size("ep")
    lane_count = lax.axis_size("tp")
    part_width = model_width // lane_count
    hidden_width = gate_proj.shape[2]
    side = EXP_GRP
    capacity = min(token_count, max(2, 2 * token_count * TOP // expert_count))
    chunk = side * capacity
    order = ORDER
    lane_index = lax.axis_index("tp")
    lane = lane_index.reshape(1)
    place = lax.axis_index("ep")
    spot = place.reshape(1)
    swap = [(number, lane_count - 1 - number) for number in range(lane_count)]
    half_type = jnp.bfloat16

    other_down = lax.ppermute(down_proj[0], "tp", swap)
    (packed,) = call(
        prepare_kernel,
        [((token_count + TOP, part_width), half_type)],
        lane,
        tokens_in,
        norm_gain.reshape(1, model_width),
        route_ids.T,
        group_weight.T,
        expert_weight.T,
        scalars=1,
        far=5,
        scratch=[
            pltpu.VMEM((token_count, model_width), half_type),
            pltpu.VMEM((1, model_width), jnp.float32),
            pltpu.VMEM((TOP, token_count), jnp.int32),
            pltpu.VMEM((group_weight.shape[1], token_count), jnp.float32),
            pltpu.VMEM((TOP, token_count), jnp.float32),
            pltpu.SemaphoreType.DMA((5,)),
        ],
    )
    blocks = [packed]
    for delta in order[1:]:
        blocks.append(shift(packed, True, delta))
    outgoing = call(
        functools.partial(select_kernel, capacity, order),
        [((chunk, part_width), half_type)] * side,
        lane,
        spot,
        *blocks,
        scalars=2,
    )
    factors, *weights = call(
        functools.partial(factors_kernel, capacity, order),
        [((side, 2 * token_count, chunk), half_type)]
        + [((model_width, hidden_width), half_type)] * 2,
        lane,
        spot,
        *blocks,
        gate_proj[0],
        up_proj[0],
        scalars=2,
        scratch=[pltpu.SemaphoreType.DMA((2,))],
        far=2,
    )
    own = [outgoing[0]]
    for place, delta in enumerate(order[1:], 1):
        own.append(shift(outgoing[place], False, delta))
    partner = []
    for delta, rows in zip(order, own):
        partner.append(lax.ppermute(rows, "tp", swap))
    late = side - EARLY

    def products(chunks, other):
        return call(
            functools.partial(half_kernel, other),
            [((len(chunks) * chunk, 2 * hidden_width), jnp.float32)],
            lane,
            *chunks,
            *weights,
            scalars=1,
        )[0]

    own_early = products(own[:EARLY], False)
    partner_early = products(partner[:EARLY], True)
    own_late = products(own[EARLY:], False)
    mine, *theirs = call(
        functools.partial(late_kernel, capacity),
        [
            ((side * chunk, hidden_width), half_type),
            ((EARLY * chunk, hidden_width), half_type),
            ((late * chunk, hidden_width), half_type),
        ],
        lane,
        *partner[EARLY:],
        *weights,
        own_early,
        partner_early,
        own_late,
        scalars=1,
        scratch=[pltpu.VMEM((late * chunk, 2 * hidden_width), jnp.float32)],
        limit=16,
    )
    near = lax.ppermute(theirs[0], "tp", swap)
    far = lax.ppermute(theirs[1], "tp", swap)
    returned = [None] * side
    for some in ((1,), tuple(range(2, EARLY)), tuple(range(EARLY, side)) + (0,)):
        results = call(
            functools.partial(down_kernel, some),
            [((chunk, part_width), half_type)] * len(some),
            lane,
            mine,
            near,
            far if some[0] >= EARLY else near,
            down_proj[0],
            other_down,
            scalars=1,
        )
        for place, result in zip(some, results):
            returned[place] = shift(result, False, -order[place]) if place else result
    kept, *partials = call(
        functools.partial(combine_kernel, capacity),
        [((token_count, part_width), jnp.float32)]
        + [((token_count, part_width), half_type)] * (side - 1),
        *returned,
        factors,
    )
    total = kept
    for place, delta in enumerate(order[1:]):
        total += shift(partials[place], True, -delta).astype(jnp.float32)
    return total.astype(half_type)


def solution(mesh):
    in_specs = (
        P(("grp", "ep"), None),
        P(),
        P("ep", None, "tp"),
        P("ep", None, "tp"),
        P("ep", "tp", None),
        P(("grp", "ep"), None),
        P(("grp", "ep"), None),
        P(("grp", "ep"), None),
    )
    out_specs = P(("grp", "ep"), "tp")
    return jax.shard_map(layer, mesh=mesh, in_specs=in_specs, out_specs=out_specs, check_vma=False)
```

```python
import functools

import jax
import jax.numpy as jnp
from jax import lax
from jax.experimental import pallas as pl
from jax.experimental.pallas import tpu as pltpu
from jax.sharding import PartitionSpec as P


TOP = 8
EXP_GRP = 8
LANES = 128

EPSILON = 1e-06
AXES = ("ep", "tp")
ORDER = (0, 4, 3, 5, 2, 6, 1, 7)
EARLY = 4


def shift_pairs(gathering, delta):
    lanes = lax.axis_size("tp")
    side = EXP_GRP
    pairs = []
    for device in range(lax.axis_size("ep")):
        row, col = divmod(device, side)
        for lane in range(lanes):
            if (lane == 0) == gathering:
                target = ((row + delta) % side) * side + col
            else:
                target = row * side + (col + delta) % side
            pairs.append((device * lanes + lane, target * lanes + lane))
    return pairs


def shift(array, gathering, delta):
    return lax.ppermute(array, AXES, shift_pairs(gathering, delta))


def call(kernel, outputs, *operands, scalars=0, scratch=(), far=0, limit=8):
    smem = pl.BlockSpec(memory_space=pltpu.SMEM)
    vmem = pl.BlockSpec(memory_space=pltpu.VMEM)
    hbm = pl.BlockSpec(memory_space=pltpu.HBM)
    near = len(operands) - far
    operands = operands[:near] + tuple(
        pltpu.with_memory_space_constraint(operand, pltpu.HBM) for operand in operands[near:]
    )
    return pl.pallas_call(
        kernel,
        out_shape=[jax.ShapeDtypeStruct(*output) for output in outputs],
        in_specs=[smem] * scalars + [vmem] * (near - scalars) + [hbm] * far,
        out_specs=[vmem] * len(outputs),
        scratch_shapes=list(scratch),
        compiler_params=pltpu.CompilerParams(vmem_limit_bytes=limit << 20),
    )(*operands)


def fdot(left, right, contract=((1,), (0,))):
    return lax.dot_general(left, right, (contract, ((), ())), preferred_element_type=jnp.float32)


def prepare_kernel(lane_ref, *refs):
    far, out_ref, near, sems = refs[:5], refs[5], refs[6:11], refs[11]
    copies = [pltpu.make_async_copy(far[n], near[n], sems.at[n]) for n in range(5)]
    for copy in copies:
        copy.start()
    for copy in copies:
        copy.wait()
    tokens_ref, gain_ref, ids_ref, group_ref, expert_ref = near
    half = out_ref.shape[1]
    count, width = tokens_ref.shape
    values = tokens_ref[...].astype(jnp.float32)
    mean = jnp.sum(values * values, axis=1, keepdims=True) / width
    scale = lax.rsqrt(mean + EPSILON)
    start = pl.multiple_of(lane_ref[0] * half, half)
    own = tokens_ref[:, pl.ds(start, half)].astype(jnp.float32)
    out_ref[:count, :] = (own * scale * gain_ref[:, pl.ds(start, half)]).astype(jnp.bfloat16)
    ids = ids_ref[...]
    group_ids = lax.div(ids, jnp.full_like(ids, EXP_GRP))
    part = jnp.zeros(ids.shape, jnp.float32)
    for group in range(group_ref.shape[0]):
        part += jnp.where(group_ids == group, group_ref[group : group + 1, :], 0.0)
    weights = expert_ref[...]
    gates = part * weights / jnp.sum(weights, axis=0, keepdims=True)
    high = gates.astype(jnp.bfloat16)
    rest = gates - high.astype(jnp.float32)
    middle = rest.astype(jnp.bfloat16)
    lowest = (rest - middle.astype(jnp.float32)).astype(jnp.bfloat16)
    out_ref[count:, :] = jnp.zeros((TOP, half), jnp.bfloat16)
    for number, term in enumerate((ids.astype(jnp.float32).astype(jnp.bfloat16), high, middle, lowest)):
        out_ref[count:, number * LANES : number * LANES + count] = term


def chosen_slots(order, lane_ref, place_ref, blocks):
    side = EXP_GRP
    tokens = blocks[0].shape[0] - TOP
    lane, place = lane_ref[0], place_ref[0]
    row, col = lax.div(place, side), lax.rem(place, side)
    line = lax.broadcasted_iota(jnp.int32, (side, tokens), 0)
    target = jnp.zeros((side, tokens), jnp.int32)
    for number, delta in enumerate(order):
        along = row * side + lax.rem(col + delta, side)
        across = lax.rem(row + delta, side) * side + col
        target = jnp.where(line == number, (1 - lane) * along + lane * across, target)
    target = target.astype(jnp.float32)
    named, gates = [], []
    for source in range(side):
        info = blocks[source][tokens:, : 4 * LANES].astype(jnp.float32)
        ids = info[:, :tokens]
        terms = [info[:, n * LANES : n * LANES + tokens] for n in range(1, 4)]
        weights = terms[0] + terms[1] + terms[2]
        match = jnp.zeros((side, tokens), jnp.float32)
        gate = jnp.zeros((side, tokens), jnp.float32)
        for choice in range(TOP):
            same = ids[choice : choice + 1, :] == target
            match = jnp.where(same, 1.0, match)
            gate = jnp.where(same, weights[choice : choice + 1, :], gate)
        named.append(match)
        gates.append(gate)
    named = jnp.concatenate(named, axis=0)
    first = lax.broadcasted_iota(jnp.int32, (tokens, tokens), 0)
    second = lax.broadcasted_iota(jnp.int32, (tokens, tokens), 1)
    before = (first < second).astype(jnp.float32).astype(jnp.bfloat16)
    rank = fdot(named.astype(jnp.bfloat16), before)
    return jnp.where(named > 0.0, rank, -1.0), gates


def select_kernel(capacity, order, lane_ref, place_ref, *refs):
    side = EXP_GRP
    blocks, outs = refs[:side], refs[side:]
    tokens = blocks[0].shape[0] - TOP
    slots, _ = chosen_slots(order, lane_ref, place_ref, blocks)
    slot = lax.broadcasted_iota(jnp.int32, (capacity, tokens), 0).astype(jnp.float32)
    for source in range(side):
        lines = [slots[source * side + n : source * side + n + 1, :] for n in range(side)]
        chosen = jnp.concatenate([(line == slot).astype(jnp.float32) for line in lines], axis=0)
        rows = fdot(chosen.astype(jnp.bfloat16), blocks[source][:tokens, :]).astype(jnp.bfloat16)
        for number in range(side):
            outs[number][source * capacity : (source + 1) * capacity, :] = rows[
                number * capacity : (number + 1) * capacity, :
            ]


def factors_kernel(capacity, order, lane_ref, place_ref, *refs):
    side = EXP_GRP
    blocks, weights = refs[:side], refs[side : side + 2]
    out_ref, held, sems = refs[side + 2], refs[side + 3 : side + 5], refs[side + 5]
    copies = [pltpu.make_async_copy(weights[n], held[n], sems.at[n]) for n in range(2)]
    for copy in copies:
        copy.start()
    tokens = blocks[0].shape[0] - TOP
    slots, gates = chosen_slots(order, lane_ref, place_ref, blocks)
    slot = lax.broadcasted_iota(jnp.int32, (capacity, tokens), 0).astype(jnp.float32)
    for source in range(side):
        factors = jnp.concatenate(
            [
                jnp.where(
                    slots[source * side + n : source * side + n + 1, :] == slot,
                    gates[source][n : n + 1, :],
                    0.0,
                )
                for n in range(side)
            ],
            axis=0,
        ).T
        high = factors.astype(jnp.bfloat16)
        out_ref[source, :tokens] = high
        out_ref[source, tokens:] = (factors - high.astype(jnp.float32)).astype(jnp.bfloat16)
    for copy in copies:
        copy.wait()


def project(chunks, weights, start, out_ref, begin):
    chunk, half = chunks[0].shape
    hidden = weights[0].shape[1]
    for first in range(0, len(chunks), 2):
        pair = chunks[first : first + 2]
        rows = jnp.concatenate([part[...] for part in pair], axis=0)
        for number, weight_ref in enumerate(weights):
            out_ref[
                begin + first * chunk : begin + (first + len(pair)) * chunk,
                number * hidden : (number + 1) * hidden,
            ] = fdot(rows, weight_ref[pl.ds(start, half), :])


def half_kernel(partner, lane_ref, *refs):
    chunks, weights, out_ref = refs[:-3], refs[-3:-1], refs[-1]
    half = chunks[0].shape[1]
    lane = 1 - lane_ref[0] if partner else lane_ref[0]
    project(chunks, weights, pl.multiple_of(lane * half, half), out_ref, 0)


def late_kernel(capacity, lane_ref, *refs):
    side = EXP_GRP
    late = side - EARLY
    partner, weights = refs[:late], refs[late : late + 2]
    own_early, partner_early, own_late, mine_ref = refs[late + 2 : late + 6]
    theirs_refs, partner_late = refs[late + 6 : late + 8], refs[late + 8]
    chunk, half = partner[0].shape
    hidden = mine_ref.shape[1]
    project(partner, weights, pl.multiple_of((1 - lane_ref[0]) * half, half), partner_late, 0)
    rows = ((0, EARLY, own_early), (EARLY, late, own_late))
    cols = ((0, EARLY, partner_early, theirs_refs[0]), (EARLY, late, partner_late, theirs_refs[1]))
    for base, count, owned in rows:
        for far_base, far_count, partnered, theirs_ref in cols:

            def block(index, carry):
                one = lax.div(index, far_count)
                two = index - one * far_count
                left = pl.multiple_of(one * chunk + (far_base + two) * capacity, capacity)
                right = pl.multiple_of(two * chunk + (base + one) * capacity, capacity)
                both = owned[pl.ds(left, capacity), :] + partnered[pl.ds(right, capacity), :]
                gate, up = both[:, :hidden], both[:, hidden:]
                acts = (gate / (1.0 + jnp.exp(-gate)) * up).astype(jnp.bfloat16)
                whole = pl.multiple_of(base * chunk + left, capacity)
                mine_ref[pl.ds(whole, capacity), :] = acts
                theirs_ref[pl.ds(right, capacity), :] = acts
                return carry

            lax.fori_loop(0, count * far_count, block, 0, unroll=4)


def down_kernel(places, lane_ref, mine_ref, near_ref, far_ref, down_ref, other_ref, *outs):
    chunk, half = outs[0].shape
    start = pl.multiple_of(lane_ref[0] * half, half)
    for place, out_ref in zip(places, outs):
        begin = place * chunk
        received_ref = far_ref if place >= EARLY else near_ref
        at = begin - EARLY * chunk if place >= EARLY else begin
        out_ref[...] = (
            fdot(mine_ref[begin : begin + chunk, :], down_ref[:, pl.ds(start, half)])
            + fdot(received_ref[at : at + chunk, :], other_ref[:, pl.ds(start, half)])
        ).astype(jnp.bfloat16)


def combine_kernel(capacity, places, *refs):
    side = EXP_GRP
    chunks, factors_ref, outs = refs[:side], refs[side], refs[side + 1 :]
    for source, out_ref in zip(places, outs):
        rows = jnp.concatenate(
            [chunk[source * capacity : (source + 1) * capacity, :] for chunk in chunks], axis=0
        )
        both = fdot(factors_ref[source], rows)
        tokens = both.shape[0] // 2
        out_ref[...] = (both[:tokens] + both[tokens:]).astype(out_ref.dtype)


def layer(
    tokens_in, norm_gain, gate_proj, up_proj, down_proj, route_ids, group_weight, expert_weight
):
    token_count, model_width = tokens_in.shape
    expert_count = gate_proj.shape[0] * lax.axis_size("ep")
    lane_count = lax.axis_size("tp")
    part_width = model_width // lane_count
    hidden_width = gate_proj.shape[2]
    side = EXP_GRP
    capacity = min(token_count, max(2, 2 * token_count * TOP // expert_count))
    chunk = side * capacity
    order = ORDER
    lane_index = lax.axis_index("tp")
    lane = lane_index.reshape(1)
    place = lax.axis_index("ep")
    spot = place.reshape(1)
    swap = [(number, lane_count - 1 - number) for number in range(lane_count)]
    half_type = jnp.bfloat16

    other_down = lax.ppermute(down_proj[0], "tp", swap)
    (packed,) = call(
        prepare_kernel,
        [((token_count + TOP, part_width), half_type)],
        lane,
        tokens_in,
        norm_gain.reshape(1, model_width),
        route_ids.T,
        group_weight.T,
        expert_weight.T,
        scalars=1,
        far=5,
        scratch=[
            pltpu.VMEM((token_count, model_width), half_type),
            pltpu.VMEM((1, model_width), jnp.float32),
            pltpu.VMEM((TOP, token_count), jnp.int32),
            pltpu.VMEM((group_weight.shape[1], token_count), jnp.float32),
            pltpu.VMEM((TOP, token_count), jnp.float32),
            pltpu.SemaphoreType.DMA((5,)),
        ],
    )
    blocks = [packed]
    for delta in order[1:]:
        blocks.append(shift(packed, True, delta))
    outgoing = call(
        functools.partial(select_kernel, capacity, order),
        [((chunk, part_width), half_type)] * side,
        lane,
        spot,
        *blocks,
        scalars=2,
    )
    factors, *weights = call(
        functools.partial(factors_kernel, capacity, order),
        [((side, 2 * token_count, chunk), half_type)]
        + [((model_width, hidden_width), half_type)] * 2,
        lane,
        spot,
        *blocks,
        gate_proj[0],
        up_proj[0],
        scalars=2,
        scratch=[pltpu.SemaphoreType.DMA((2,))],
        far=2,
    )
    own = [outgoing[0]]
    for place, delta in enumerate(order[1:], 1):
        own.append(shift(outgoing[place], False, delta))
    partner = []
    for delta, rows in zip(order, own):
        partner.append(lax.ppermute(rows, "tp", swap))
    late = side - EARLY

    def products(chunks, other):
        return call(
            functools.partial(half_kernel, other),
            [((len(chunks) * chunk, 2 * hidden_width), jnp.float32)],
            lane,
            *chunks,
            *weights,
            scalars=1,
        )[0]

    own_early = products(own[:EARLY], False)
    partner_early = products(partner[:EARLY], True)
    own_late = products(own[EARLY:], False)
    mine, *theirs = call(
        functools.partial(late_kernel, capacity),
        [
            ((side * chunk, hidden_width), half_type),
            ((EARLY * chunk, hidden_width), half_type),
            ((late * chunk, hidden_width), half_type),
        ],
        lane,
        *partner[EARLY:],
        *weights,
        own_early,
        partner_early,
        own_late,
        scalars=1,
        scratch=[pltpu.VMEM((late * chunk, 2 * hidden_width), jnp.float32)],
        limit=16,
    )
    near = lax.ppermute(theirs[0], "tp", swap)
    far = lax.ppermute(theirs[1], "tp", swap)
    returned = [None] * side
    for some in ((1,), tuple(range(2, EARLY)), tuple(range(EARLY, side)) + (0,)):
        results = call(
            functools.partial(down_kernel, some),
            [((chunk, part_width), half_type)] * len(some),
            lane,
            mine,
            near,
            far if some[0] >= EARLY else near,
            down_proj[0],
            other_down,
            scalars=1,
        )
        for place, result in zip(some, results):
            returned[place] = shift(result, False, -order[place]) if place else result
    partials = [None] * side
    for some in ((1,), (0,) + tuple(range(2, side))):
        sums = call(
            functools.partial(combine_kernel, capacity, some),
            [((token_count, part_width), half_type if place else jnp.float32) for place in some],
            *returned,
            factors,
        )
        for place, partial in zip(some, sums):
            partials[place] = partial
    total = partials[0]
    for place, delta in enumerate(order[1:], 1):
        total += shift(partials[place], True, -delta).astype(jnp.float32)
    return total.astype(half_type)


def solution(mesh):
    in_specs = (
        P(("grp", "ep"), None),
        P(),
        P("ep", None, "tp"),
        P("ep", None, "tp"),
        P("ep", "tp", None),
        P(("grp", "ep"), None),
        P(("grp", "ep"), None),
        P(("grp", "ep"), None),
    )
    out_specs = P(("grp", "ep"), "tp")
    return jax.shard_map(layer, mesh=mesh, in_specs=in_specs, out_specs=out_specs, check_vma=False)
```
